32 devices in a mesh: grp: 2 (over y), sp: 4 (over z), dp: 4 (over x, core).
Axes of the slice: x: 2, y: 2, z: 4, core: 2. Of those that a mesh axis runs over, the one named last changes fastest.
Arguments:
- mixer_source_array: bfloat16 [8, 768, 2048], P(('grp', 'dp'), 'sp'), parts along dimension 0, may hold values from -6 to 6
- source_projection: bfloat16 [2048, 1024], P('dp'), may hold values from -0.125 to 0.125
- gating_projection: bfloat16 [2048, 1024], P('dp'), may hold values from -0.125 to 0.125
- entry_mapping_projection: bfloat16 [2048, 256], replicated, may hold values from -0.0390625 to 0.0390625
- readout_mapping_projection: bfloat16 [2048, 256], replicated, may hold values from -0.0390625 to 0.0390625
- increment_projection: bfloat16 [2048, 16], replicated, may hold values from -0.125 to 0.125
- source_conv_taps: float32 [4, 1024], replicated, may hold values from -3 to 3
- entry_mapping_taps: float32 [4, 256], replicated, may hold values from -3 to 3
- readout_mapping_taps: float32 [4, 256], replicated, may hold values from -3 to 3
- increment_offsets: float32 [16], replicated, may hold values from -1 to 1
- channel_damping_rate: float32 [16], replicated, may hold values from 0 to 1
- bypass_coefficients: float32 [16], replicated, may hold values from 0.5 to 1.5
- stride_multiplier: float32 [8, 768], P(('grp', 'dp')), parts along dimension 0, may hold values from 0.5 to 2
- added_log_damping: float32 [8, 768, 16], P(('grp', 'dp')), parts along dimension 0, may hold values from -2.1 to 0
- norm_scale_factor: float32 [1024], replicated, may hold values from 0.1 to 1.9
- final_projection: bfloat16 [1024, 2048], P(None, 'dp'), may hold values from -0.1875 to 0.1875
Outputs:
- output: bfloat16 [8, 768, 2048], P(('grp', 'dp'), 'sp'), parts along dimension 0
The draws below stay inside these ranges and needn't reach their ends.
There are 2 independent parts, one for each index of `grp`. The reference program is written for one: setup_inputs(seed, part) draws one part's arguments, and reference() takes and returns one part's arrays. A program takes and returns all parts, laid end to end along the dimension named above; an argument that names none is the same for every part. Nothing has to cross between parts.
All inputs are finite; a program needn't handle non-finite values.
Results may differ from the reference program's by a relative error of at most 0.015.
Values may be sent and summed in bfloat16 or wider, within the bound.
No kernel may reach another device: no remote copies, remote signals or barrier semaphores. Data moves between devices by JAX's collectives and lax.ppermute only.
A program may use at most 64 MiB of HBM per device.

```python
import math
import jax
import jax.numpy as jnp
from jax import lax

D = 2048
H = 16
P_SIZE = 64
N = 128
G = 2
CONV_W = 4
BLK = 64
TOK_DEV = 192
LEN = 768
SEQS = 4


def draw_channel_damping_rate(key, part):
    base = jax.random.fold_in(key, 101)
    key_kind, key_fast, key_slow = jax.random.split(base, 3)
    fast_share = 0.5
    fast_mask = jax.random.uniform(key_kind, (H,), jnp.float32) < fast_share
    fast_rate = jax.random.uniform(key_fast, (H,), jnp.float32, math.log(1.5 / BLK), math.log(2.5 / BLK))
    slow_rate = jax.random.uniform(key_slow, (H,), jnp.float32, math.log(0.1 / LEN), math.log(0.8 / LEN))
    return jnp.exp(jnp.where(fast_mask, fast_rate, slow_rate))


def draw_stride_multiplier(key, part):
    base = jax.random.fold_in(key, 202)
    shards = LEN // TOK_DEV
    factors = jnp.exp(jax.random.uniform(base, (SEQS, shards), jnp.float32, math.log(0.5), math.log(2.0)))
    return jnp.repeat(factors, TOK_DEV, axis=1)


def draw_added_log_damping(key, part):
    base = jax.random.fold_in(key, 303)
    key_spot, key_loss = jax.random.split(base, 2)
    spots = jax.random.randint(key_spot, (SEQS, 3), 0, LEN)
    losses = jax.random.uniform(key_loss, (SEQS, 3, H), jnp.float32, math.log(0.5), math.log(0.8))
    marks = (jnp.arange(LEN)[None, None, :] == spots[:, :, None]).astype(jnp.float32)
    return jnp.einsum('sbl,sbh->slh', marks, losses)


def steps_of(own_key, dims, pieces, least, top_value):
    factor_of, own = 1.0, jax.random.fold_in(own_key, 6)
    for axis_at, shards_of in pieces:
        heights = jnp.exp(jax.random.uniform(jax.random.fold_in(own, axis_at), (shards_of,), jnp.float32, least / len(pieces), top_value / len(pieces)))
        factor_of = factor_of * jnp.repeat(heights, dims[axis_at] // shards_of).reshape([-1 if axis == axis_at else 1 for axis in range(len(dims))])
    return factor_of


def centred(rng, shape, deviation, reach, pieces=(), kind=jnp.bfloat16):
    gain = steps_of(rng, shape, pieces, -0.22, 0.18) if pieces else 1.0
    drawn = jax.random.normal(rng, shape, jnp.float32) * deviation * gain
    return jnp.minimum(jnp.maximum(drawn, -reach), reach).astype(kind)


def setup_inputs(seed: int = 0, part: int = 0) -> dict:
    key_of = jax.random.split(jax.random.key(seed), 17)
    part_keys = jax.random.split(jax.random.fold_in(key_of[16], part), 17)
    return {
        "mixer_source_array": centred(part_keys[0], (SEQS, LEN, D), 1.0, 6.0, ((0, 4), (1, 4))),
        "source_projection": centred(key_of[1], (D, H * P_SIZE), D ** -0.5, 0.125, ((0, 4),)),
        "gating_projection": centred(key_of[2], (D, H * P_SIZE), D ** -0.5, 0.125, ((0, 4),)),
        "entry_mapping_projection": centred(key_of[3], (D, G * N), (10 * D) ** -0.5, 0.0390625),
        "readout_mapping_projection": centred(key_of[4], (D, G * N), (10 * D) ** -0.5, 0.0390625),
        "increment_projection": centred(key_of[5], (D, H), D ** -0.5, 0.125),
        "source_conv_taps": centred(key_of[6], (CONV_W, H * P_SIZE), CONV_W ** -0.5, 3.0, (), jnp.float32),
        "entry_mapping_taps": centred(key_of[7], (CONV_W, G * N), CONV_W ** -0.5, 3.0, (), jnp.float32),
        "readout_mapping_taps": centred(key_of[8], (CONV_W, G * N), CONV_W ** -0.5, 3.0, (), jnp.float32),
        "increment_offsets": jnp.clip(jax.random.uniform(key_of[9], (H,), jnp.float32, -1.0, 1.0), -1.0, 1.0),
        "channel_damping_rate": draw_channel_damping_rate(jax.random.fold_in(key_of[16], 71), part),
        "bypass_coefficients": jnp.clip(jax.random.uniform(key_of[11], (H,), jnp.float32, 0.5, 1.5), 0.5, 1.5),
        "stride_multiplier": draw_stride_multiplier(jax.random.fold_in(jax.random.fold_in(key_of[16], part), 71), part),
        "added_log_damping": draw_added_log_damping(jax.random.fold_in(jax.random.fold_in(key_of[16], part), 71), part),
        "norm_scale_factor": jnp.clip(1.0 + 0.18 * jax.random.normal(key_of[14], (H * P_SIZE,), jnp.float32), 0.1, 1.9),
        "final_projection": centred(key_of[15], (H * P_SIZE, D), (H * P_SIZE) ** -0.5, 0.1875, ((1, 4),)),
    }


EPSILON = 1e-06
HIGH = lax.Precision.HIGHEST

def conv_silu(padded, taps):
    width = taps.shape[0]
    length = padded.shape[0] - width + 1
    total = taps[0][None, :] * padded[0:length]
    for shift_pos in range(1, width):
        total = total + taps[shift_pos][None, :] * padded[shift_pos:shift_pos + length]
    return jax.nn.silu(total).astype(jnp.bfloat16)

def block_parts(x_blocks, b_blocks, c_blocks, step_width_value, logarithm_retain):
    cumulative = jnp.cumsum(logarithm_retain, axis=1)
    scaled = (x_blocks.astype(jnp.float32) * step_width_value[..., None]).astype(jnp.bfloat16)
    intersection = jnp.einsum('kign,kjgn->kgij', c_blocks.astype(jnp.float32), b_blocks.astype(jnp.float32), precision=HIGH)
    by_row = jnp.transpose(cumulative, (0, 2, 3, 1))
    log_gap = by_row[..., :, None] - by_row[..., None, :]
    length = log_gap.shape[-1]
    lower = jnp.tril(jnp.ones((length, length), bool))
    mixing = (intersection[:, :, None] * jnp.exp(jnp.where(lower, log_gap, -jnp.inf))).astype(jnp.bfloat16)
    inner = jnp.einsum('kgrij,kjgrp->kigrp', mixing.astype(jnp.float32), scaled.astype(jnp.float32), precision=HIGH)
    to_end = jnp.exp(cumulative[:, -1:] - cumulative)
    weighted = (b_blocks[:, :, :, None, :].astype(jnp.float32) * to_end[..., None]).astype(jnp.bfloat16)
    states = jnp.einsum('kjgrn,kjgrp->kgrnp', weighted.astype(jnp.float32), scaled.astype(jnp.float32), precision=HIGH)
    return (inner, states, cumulative[:, -1], cumulative)

def block_carry(states, block_total):
    incl_sum = jnp.cumsum(block_total, axis=0)
    excl_sum = incl_sum - block_total
    count = block_total.shape[0]
    log_gap = excl_sum[:, None] - incl_sum[None, :]
    before = (jnp.arange(count)[None, :] < jnp.arange(count)[:, None])[:, :, None, None]
    factors = jnp.exp(jnp.where(before, log_gap, -jnp.inf))
    carried = jnp.einsum('kjgr,jgrnp->kgrnp', factors, states, precision=HIGH)
    return carried

def block_finish(inner, c_blocks, cumulative, carried, x_blocks, skip):
    reached = jnp.einsum('kign,kgrnp->kigrp', c_blocks.astype(jnp.float32), carried, precision=HIGH)
    return inner + reached * jnp.exp(cumulative)[..., None] + skip[..., None] * x_blocks.astype(jnp.float32)

def reference(mixer_source_array, source_projection, gating_projection, entry_mapping_projection, readout_mapping_projection, increment_projection, source_conv_taps, entry_mapping_taps, readout_mapping_taps, increment_offsets, channel_damping_rate, bypass_coefficients, stride_multiplier, added_log_damping, norm_scale_factor, final_projection):
    per_group = H // G
    blocks = LEN // BLK

    def lone_stream_case(input_rows):
        hidden_width, tempo_row_values, surge_row_values = input_rows
        proj_x = jnp.dot(hidden_width, source_projection, preferred_element_type=jnp.float32).astype(jnp.bfloat16)
        gate_z = jnp.dot(hidden_width, gating_projection, preferred_element_type=jnp.float32).astype(jnp.bfloat16)
        proj_b = jnp.dot(hidden_width, entry_mapping_projection, preferred_element_type=jnp.float32).astype(jnp.bfloat16)
        proj_c = jnp.dot(hidden_width, readout_mapping_projection, preferred_element_type=jnp.float32).astype(jnp.bfloat16)
        step_raw = jnp.dot(hidden_width, increment_projection, preferred_element_type=jnp.float32).astype(jnp.bfloat16)
        xs = conv_silu(jnp.concatenate([jnp.zeros((CONV_W - 1, H * P_SIZE), jnp.float32), proj_x.astype(jnp.float32)], 0), source_conv_taps)
        bm = conv_silu(jnp.concatenate([jnp.zeros((CONV_W - 1, G * N), jnp.float32), proj_b.astype(jnp.float32)], 0), entry_mapping_taps)
        cm = conv_silu(jnp.concatenate([jnp.zeros((CONV_W - 1, G * N), jnp.float32), proj_c.astype(jnp.float32)], 0), readout_mapping_taps)
        step_width_value = jax.nn.softplus(step_raw.astype(jnp.float32) + increment_offsets[None, :])
        logarithm_retain = -channel_damping_rate[None, :] * step_width_value * tempo_row_values[:, None] + surge_row_values
        x_blocks = xs.reshape(blocks, BLK, G, per_group, P_SIZE)
        b_blocks = bm.reshape(blocks, BLK, G, N)
        c_blocks = cm.reshape(blocks, BLK, G, N)
        inner, states, block_total, cumulative = block_parts(x_blocks, b_blocks, c_blocks, step_width_value.reshape(blocks, BLK, G, per_group), logarithm_retain.reshape(blocks, BLK, G, per_group))
        carried = block_carry(states, block_total)
        mixed = block_finish(inner, c_blocks, cumulative, carried, x_blocks, bypass_coefficients.reshape(G, per_group))
        mixed = mixed.astype(jnp.bfloat16).reshape(LEN, H * P_SIZE)
        gated = mixed.astype(jnp.float32) * jax.nn.silu(gate_z.astype(jnp.float32))
        grouped = gated.reshape(LEN, G, H * P_SIZE // G)
        normed = grouped * lax.rsqrt(lax.optimization_barrier(jnp.mean(grouped * grouped, axis=-1, keepdims=True)) + EPSILON)
        normed = (normed.reshape(LEN, H * P_SIZE) * norm_scale_factor[None, :]).astype(jnp.bfloat16)
        return jnp.dot(normed, final_projection, preferred_element_type=jnp.float32).astype(jnp.bfloat16)
    return lax.map(lone_stream_case, (mixer_source_array, stride_multiplier, added_log_damping))
```

```python
import functools

import jax
import jax.numpy as jnp
from jax import lax
from jax.experimental import pallas as pl
from jax.experimental.pallas import tpu as pltpu
from jax.sharding import PartitionSpec as P


N = 128
G = 2
HALO = 16
EPSILON = 1e-06
HIGH = lax.Precision.HIGHEST
F32 = jnp.float32
BF16 = jnp.bfloat16
SDS = jax.ShapeDtypeStruct


def dot(a, b, precision=None):
    return jnp.dot(a, b, preferred_element_type=F32, precision=precision)


def dot_t(a, b):
    return lax.dot_general(a, b, (((1,), (1,)), ((), ())), preferred_element_type=F32)


def dot_tl(a, b, precision=None):
    return lax.dot_general(
        a, b, (((0,), (0,)), ((), ())), preferred_element_type=F32, precision=precision
    )


def silu(v):
    return v / (1.0 + jnp.exp(-v))


def conv_silu(ref, first, taps, rows):
    width = taps.shape[0]
    first = first + HALO - (width - 1)
    total = taps[0:1, :] * ref[pl.ds(first, rows), :]
    for k in range(1, width):
        total = total + taps[k : k + 1, :] * ref[pl.ds(first + k, rows), :]
    return silu(total).astype(BF16)


def aligned(index, size):
    return pl.ds(pl.multiple_of(index * size, size), size)


def my_group():
    return lax.rem(lax.axis_index("dp"), G)


def maps_kernel(
    x_ref,
    wb_ref,
    wc_ref,
    wdt_ref,
    taps_b_ref,
    taps_c_ref,
    offset_ref,
    rate_ref,
    stride0_ref,
    stride1_ref,
    added0_ref,
    added1_ref,
    bm_ref,
    cm_ref,
    mix_ref,
    step_ref,
    send_ref,
    reach_ref,
    total_ref,
    pad_ref,
):
    c = my_group()
    place = lax.axis_index("sp")
    spans = lax.axis_size("sp")
    full = x_ref.shape[0] // 2
    rows = full - HALO
    heads = wdt_ref.shape[0] // G
    width = step_ref.shape[1]
    mine = aligned(c, N)
    for w_ref, taps_ref, out_ref in ((wb_ref, taps_b_ref, bm_ref), (wc_ref, taps_c_ref, cm_ref)):
        pad_ref[...] = dot(x_ref[...], w_ref[:, mine]).astype(BF16).astype(F32)
        for q in range(2):
            out_ref[q * rows : (q + 1) * rows, :] = conv_silu(
                pad_ref, q * full, taps_ref[:, mine], rows
            )
    src = lax.broadcasted_iota(jnp.int32, (rows, rows), 0)
    dst = lax.broadcasted_iota(jnp.int32, (rows, rows), 1)
    upper = (src <= dst).astype(F32)
    eye = (
        lax.broadcasted_iota(jnp.int32, (heads, heads), 0)
        == lax.broadcasted_iota(jnp.int32, (heads, heads), 1)
    ).astype(F32)
    spread = (
        lax.broadcasted_iota(jnp.int32, (heads, width), 1) // (width // heads)
        == lax.broadcasted_iota(jnp.int32, (heads, width), 0)
    ).astype(F32)
    head = lax.broadcasted_iota(jnp.int32, (heads, 1), 0)
    offset = jnp.zeros((heads, 1), F32)
    rate = jnp.zeros((heads, 1), F32)
    for r in range(heads):
        offset = jnp.where(head == r, offset_ref[c * heads + r], offset)
        rate = jnp.where(head == r, rate_ref[c * heads + r], rate)
    wdt = wdt_ref[aligned(c, heads), :]

    def own_span(ref, sub):
        picked = ref[sub, 0:rows]
        for s in range(1, spans):
            picked = jnp.where(place == s, ref[sub, s * rows : (s + 1) * rows], picked)
        return picked

    for q, (stride_ref, added_ref) in enumerate(
        ((stride0_ref, added0_ref), (stride1_ref, added1_ref))
    ):
        out = slice(q * rows, (q + 1) * rows)
        x_rows = x_ref[q * full + HALO : (q + 1) * full, :]
        raw = dot_t(wdt, x_rows).astype(BF16).astype(F32)
        shifted = raw + offset
        step_t = jnp.maximum(shifted, 0.0) + jnp.log1p(jnp.exp(-jnp.abs(shifted)))
        stride = own_span(stride_ref, slice(0, 1))
        added = own_span(added_ref, aligned(c, heads))
        keep_t = -rate * step_t * stride + added
        cum_t = dot(keep_t, upper, HIGH)
        total_t = cum_t[:, rows - 1 : rows]
        cum = dot_tl(cum_t, eye, HIGH)
        step_ref[out, :] = dot_tl(step_t, spread, HIGH)
        send_ref[out, :] = dot_tl(step_t * jnp.exp(total_t - cum_t), spread, HIGH)
        reach_ref[out, :] = dot_tl(jnp.exp(cum_t), spread, HIGH)
        total_ref[q * 8 : (q + 1) * 8, :] = dot_tl(
            jnp.broadcast_to(total_t, (heads, 8)), spread, HIGH
        )
        gram = jnp.where(src >= dst, dot_t(cm_ref[out, :], bm_ref[out, :]), 0.0)
        for r in range(heads):
            gap = cum[:, r : r + 1] - cum_t[r : r + 1, :]
            mix_ref[q * heads + r] = (gram * jnp.exp(jnp.minimum(gap, 0.0))).astype(BF16)


def shard_of(shift, flip):
    size = lax.axis_size("dp")
    return lax.rem(lax.axis_index("dp") - shift + size, size) ^ flip


def half_of(part):
    g = lax.axis_index("grp")
    return g if part == 0 else 1 - g


def proj_pieces(x_ref, refs, kinds, rows_w):
    total = None
    c = my_group()
    for ref, (shift, flip, part) in zip(refs, kinds):
        depth, lanes = ref.shape
        index = shard_of(shift, flip) * (rows_w // depth)
        if part is not None:
            index = index + half_of(part)
        w = ref[...] if (shift, flip) != (0, 0) else ref[:, aligned(c, lanes // G)]
        piece = dot(x_ref[:, aligned(index, depth)], w)
        total = piece if total is None else total + piece
    return total


def source_kernel(kinds, rows_w, *refs):
    x_ref, taps_ref, step_ref, send_ref, bm_ref = refs[:5]
    pieces = refs[5 : 5 + len(kinds)]
    xs_ref, scaled_ref, state_ref, state_bf_ref, pad_ref = refs[5 + len(kinds) :]
    full = x_ref.shape[0] // 2
    rows = full - HALO
    pad_ref[...] = proj_pieces(x_ref, pieces, kinds, rows_w).astype(BF16).astype(F32)
    taps = taps_ref[:, aligned(my_group(), pad_ref.shape[1])]
    for q in range(2):
        out = slice(q * rows, (q + 1) * rows)
        xs = conv_silu(pad_ref, q * full, taps, rows)
        xs_ref[out, :] = xs
        wide = xs.astype(F32)
        sent = (wide * send_ref[out, :]).astype(BF16)
        state = dot_tl(bm_ref[out, :], sent)
        state_ref[q * N : (q + 1) * N, :] = state
        state_bf_ref[q * N : (q + 1) * N, :] = state.astype(BF16)
        scaled_ref[out, :] = (wide * step_ref[out, :]).astype(BF16)


def gate_kernel(kinds, rows_w, *refs):
    x_ref = refs[0]
    pieces = refs[1 : 1 + len(kinds)]
    out_ref = refs[1 + len(kinds)]
    full = x_ref.shape[0] // 2
    z = silu(proj_pieces(x_ref, pieces, kinds, rows_w).astype(BF16).astype(F32))
    for q in range(2):
        out_ref[q * (full - HALO) : (q + 1) * (full - HALO), :] = z[q * full + HALO : (q + 1) * full]


def local_kernel(mix_ref, scaled_ref, xs_ref, skip_ref, out_ref):
    heads = mix_ref.shape[0] // 2
    rows = mix_ref.shape[1]
    size = scaled_ref.shape[1] // heads
    pack = max(1, 128 // size)
    first = my_group() * heads
    for q in range(2):
        out = slice(q * rows, (q + 1) * rows)
        for p in range(heads // pack):
            lanes = slice(p * pack * size, (p + 1) * pack * size)
            data = scaled_ref[out, lanes]
            where = lax.broadcasted_iota(jnp.int32, data.shape, 1) // size
            skip = jnp.zeros(data.shape, F32)
            total = None
            for r in range(pack):
                h = p * pack + r
                skip = jnp.where(where == r, skip_ref[first + h], skip)
                own = jnp.where(where == r, data, jnp.zeros_like(data))
                part = dot(mix_ref[q * heads + h], own)
                total = part if total is None else total + part
            out_ref[out, lanes] = total + skip * xs_ref[out, lanes].astype(F32)


def finish_kernel(kinds, cols, n_recv, slot, *refs):
    local_ref, cm_ref, reach_ref, gate_ref, scale_ref = refs[:5]
    recv = refs[5 : 5 + n_recv]
    decay = refs[5 + n_recv : 4 + 2 * n_recv]
    pieces = refs[4 + 2 * n_recv : 4 + 2 * n_recv + len(kinds)]
    out_ref, normed_ref = refs[4 + 2 * n_recv + len(kinds) :]
    rows = local_ref.shape[0] // 2
    width = local_ref.shape[1]
    c = my_group()
    mine = slice(slot * rows, (slot + 1) * rows)
    states = slice(slot * N, (slot + 1) * N)
    carry = recv[0][states, :].astype(F32)
    for r_ref, d_ref in zip(recv[1:], decay):
        carry = carry + r_ref[states, :].astype(F32) * d_ref[slot * 8 : slot * 8 + 1, :]
    reached = dot(cm_ref[mine, :], carry.astype(BF16))
    mixed = (local_ref[mine, :] + reached * reach_ref[mine, :]).astype(BF16)
    gated = mixed.astype(F32) * gate_ref[mine, :]
    mean = jnp.mean(gated * gated, axis=-1, keepdims=True)
    normed = gated * lax.rsqrt(mean + EPSILON)
    normed_ref[...] = (normed * scale_ref[:, aligned(c, width)]).astype(BF16)
    groups = {}
    for ref, (shift, flip, part) in zip(pieces, kinds):
        groups.setdefault((shift, flip), []).append((ref, part))
    for (shift, flip), members in groups.items():
        total = None
        for ref, part in members:
            if part is None:
                left = normed_ref[...]
            else:
                left = normed_ref[:, aligned(half_of(part), ref.shape[0])]
            w = ref[...] if (shift, flip) != (0, 0) else ref[aligned(c, width), :]
            piece = dot(left, w)
            total = piece if total is None else total + piece
        out_ref[:, aligned(shard_of(shift, flip), cols)] = total.astype(out_ref.dtype)


def permute(v, axis, pairs):
    return lax.ppermute(v, axis, pairs)


def gather_pieces(own, dim):
    size = lax.axis_size("dp")
    rows = own.shape[0] // (G if dim == 0 else 1)
    lanes = own.shape[1] // (G if dim == 1 else 1)
    share = lax.axis_size("grp") == 2 and rows % 256 == 0
    g = lax.axis_index("grp")
    c = my_group()

    def part(group, whole):
        at = [0, 0]
        at[dim] = group * (own.shape[dim] // G)
        depth = rows
        if share and not whole:
            depth = rows // 2
            at[0] = at[0] + g * depth
        return lax.dynamic_slice(own, at, (depth, lanes))

    pieces = [own, permute(part(1 - c, True), "dp", [(i, i ^ 1) for i in range(size)])]
    kinds = [(0, 0, None), (0, 1, None)]
    for r in range(1, size // 2):
        for flip in range(2):
            pairs = [(i, (i ^ flip) + 2 * r - size * ((i ^ flip) + 2 * r >= size)) for i in range(size)]
            a = permute(part(c ^ flip, False), "dp", pairs)
            pieces.append(a)
            if share:
                b = permute(a, "grp", [(0, 1), (1, 0)])
                pieces.append(b)
                kinds += [(2 * r, flip, 0), (2 * r, flip, 1)]
            else:
                kinds += [(2 * r, flip, None)]
    return pieces, tuple(kinds)


def call(kernel, outs, *args, scratch=(), flops=1000000, smem=()):
    specs = [
        pl.BlockSpec(memory_space=pltpu.SMEM if i in smem else pltpu.VMEM)
        for i in range(len(args))
    ]
    args = [
        v if i in smem else pltpu.with_memory_space_constraint(v, pltpu.VMEM)
        for i, v in enumerate(args)
    ]
    many = isinstance(outs, tuple)
    shapes = tuple(pltpu.VMEM(v.shape, v.dtype) for v in (outs if many else (outs,)))
    return pl.pallas_call(
        kernel,
        out_shape=shapes if many else shapes[0],
        compiler_params=pltpu.CompilerParams(vmem_limit_bytes=24 << 20),
        in_specs=specs,
        scratch_shapes=scratch,
        cost_estimate=pl.CostEstimate(flops=flops, transcendentals=0, bytes_accessed=1000000),
    )(*args)


def shards(
    mixer_source_array,
    source_projection,
    gating_projection,
    entry_mapping_projection,
    readout_mapping_projection,
    increment_projection,
    source_conv_taps,
    entry_mapping_taps,
    readout_mapping_taps,
    increment_offsets,
    channel_damping_rate,
    bypass_coefficients,
    stride_multiplier,
    added_log_damping,
    norm_scale_factor,
    final_projection,
):
    x = mixer_source_array[0]
    rows = x.shape[0]
    heads = increment_projection.shape[1] // G
    width = source_projection.shape[1] // G
    spans = lax.axis_size("sp")
    pair = [(i, i ^ 1) for i in range(lax.axis_size("dp"))]

    def forward(v, k):
        return permute(v, "sp", [(i, i + k) for i in range(spans - k)])

    src_pieces, src_kinds = gather_pieces(source_projection, 1)
    halo = forward(x[rows - HALO :], 1)
    added = added_log_damping[0].T
    added_pair = permute(added, "dp", pair)
    stride_pair = permute(stride_multiplier, "dp", pair)
    x_own = jnp.concatenate([halo, x], 0)
    x_pair = jnp.concatenate([x_own, permute(x_own, "dp", pair)], 0)

    gate_pieces, gate_kinds = gather_pieces(gating_projection, 1)
    out_pieces, out_kinds = gather_pieces(final_projection, 0)

    bm, cm, mix, step, send, reach, total = call(
        maps_kernel,
        (
            SDS((2 * rows, N), BF16),
            SDS((2 * rows, N), BF16),
            SDS((2 * heads, rows, rows), BF16),
            SDS((2 * rows, width), F32),
            SDS((2 * rows, width), F32),
            SDS((2 * rows, width), F32),
            SDS((16, width), F32),
        ),
        x_pair,
        entry_mapping_projection,
        readout_mapping_projection,
        increment_projection.T,
        entry_mapping_taps,
        readout_mapping_taps,
        increment_offsets,
        channel_damping_rate,
        stride_multiplier,
        stride_pair,
        added,
        added_pair,
        scratch=(pltpu.VMEM((2 * (rows + HALO), N), F32),),
        flops=4000000000,
        smem=(6, 7),
    )
    state_shape = (2 * N, width)
    xs, scaled, state, state_bf = call(
        functools.partial(source_kernel, src_kinds, source_projection.shape[0]),
        (
            SDS((2 * rows, width), BF16),
            SDS((2 * rows, width), BF16),
            SDS(state_shape, F32),
            SDS(state_shape, BF16),
        ),
        x_pair,
        source_conv_taps,
        step,
        send,
        bm,
        *src_pieces,
        scratch=(pltpu.VMEM((2 * (rows + HALO), width), F32),),
        flops=2000000000,
    )

    def spread_rows(v):
        factors = jnp.exp(v.reshape(2, 8, width)[:, :1])
        return jnp.broadcast_to(factors, (2, N, width)).reshape(state_shape)

    received = []
    decays = []
    window = total
    behind = None
    inclusive, inclusive_bf = state, state_bf
    k = 1
    while k < spans:
        arrived = forward(inclusive_bf, k)
        received.append(arrived)
        if behind is not None:
            decays.append(jnp.exp(behind))
        if 2 * k < spans:
            far = forward(window, k)
            inclusive = inclusive + spread_rows(window) * arrived.astype(F32)
            inclusive_bf = inclusive.astype(BF16)
            behind = far if behind is None else behind + far
            window = window + far
        k *= 2

    gate = call(
        functools.partial(gate_kernel, gate_kinds, gating_projection.shape[0]),
        SDS((2 * rows, width), F32),
        x_pair,
        *gate_pieces,
        flops=2000000000,
    )
    local = call(
        local_kernel,
        SDS((2 * rows, width), F32),
        mix,
        scaled,
        xs,
        bypass_coefficients,
        flops=3000000000,
        smem=(3,),
    )

    def finish(slot, kind):
        cols = final_projection.shape[1]
        return call(
            functools.partial(finish_kernel, out_kinds, cols, len(received), slot),
            SDS((rows, cols * lax.axis_size("dp")), kind),
            local,
            cm,
            reach,
            gate,
            norm_scale_factor[None, :],
            *received,
            *decays,
            *out_pieces,
            scratch=(pltpu.VMEM((rows, width), BF16),),
            flops=2000000000,
        )

    other = permute(finish(1, BF16), "dp", pair)
    output = (finish(0, F32) + other.astype(F32)).astype(BF16)
    return output[None]


def solution(mesh):
    return jax.shard_map(
        shards,
        mesh=mesh,
        in_specs=(
            P(("grp", "dp"), "sp", None),
            P("dp", None),
            P("dp", None),
            P(),
            P(),
            P(),
            P(),
            P(),
            P(),
            P(),
            P(),
            P(),
            P(("grp", "dp"), None),
            P(("grp", "dp"), None, None),
            P(),
            P(None, "dp"),
        ),
        out_specs=P(("grp", "dp"), "sp", None),
        check_vma=False,
    )
```
